128 devices in a mesh: kv: 16 (over z, x), tp: 8 (over y, core).
Axes of the slice: x: 4, y: 4, z: 4, core: 2. Of those that a mesh axis runs over, the one named last changes fastest.
Arguments:
- hidden_in: bfloat16 [16, 4096], P(None, ('kv', 'tp')), may hold values from -5 to 5
- pre_gain: float32 [4096], P('kv'), may hold values from 0.1 to 1.9
- w_query: bfloat16 [4096, 3072], P('kv', 'tp'), may hold values from -0.09375 to 0.09375
- w_key: bfloat16 [4096, 1024], P('kv', 'tp'), may hold values from -0.09375 to 0.09375
- w_value: bfloat16 [4096, 1024], P('kv', 'tp'), may hold values from -0.09375 to 0.09375
- w_forget: bfloat16 [4096, 16], P('kv'), may hold values from -0.09375 to 0.09375
- forget_bias: float32 [16], P('tp'), may hold values from -2 to 1.5
- key_cache: bfloat16 [16, 16384, 1024], P(None, 'kv', 'tp'), may hold values from -1300 to 1300
- value_cache: bfloat16 [16, 16384, 1024], P(None, 'kv', 'tp'), may hold values from -6 to 6
- decay_to_end: float32 [16, 16, 16384], P(None, 'tp', 'kv'), may hold values from -16386 to 0, as said below
- w_output: bfloat16 [3072, 4096], P('tp', 'kv'), may hold values from -0.109375 to 0.109375
- mid_gain: float32 [4096], P('kv'), may hold values from 0.1 to 1.9
- w_gate: bfloat16 [4096, 11264], P('kv', 'tp'), may hold values from -0.09375 to 0.09375
- w_up: bfloat16 [4096, 11264], P('kv', 'tp'), may hold values from -0.09375 to 0.09375
- w_down: bfloat16 [11264, 4096], P('tp', 'kv'), may hold values from -0.0546875 to 0.0546875
Outputs:
- updated: float32 [16, 4096], P(None, ('kv', 'tp'))
The draws below stay inside these ranges and needn't reach their ends.
Inputs may be any that keep to these rules, and one draw needn't show every extreme that they name: `decay_to_end`: never falls toward later positions and is 0 at the last cached position.
All inputs are finite; a program needn't handle non-finite values.
Results may differ from the reference program's by a relative error of at most 0.028.
Values may be sent and summed in bfloat16 or wider, within the bound.
A program may use at most 64 MiB of HBM per device.

```python
import jax
import jax.numpy as jnp
from jax import lax

D = 4096
QH = 48
KEY_VALUE_HEADS = 16
HD = 64
FF = 11264
BATCH_SEQUENCES = 16
POS_DEV = 1024
CACHE_LENGTH = 16384
N_KV = 16
N_TP = 8


def draw_hidden_in(key, part):
    key_base, key_rough = jax.random.split(key, 2)
    column = jnp.arange(D).astype(jnp.float32)
    span = D // N_KV
    rise = column / D + column % span / span
    rough = jnp.exp(jax.random.uniform(key_rough, (D,), minval=-0.7, maxval=0.7))
    scale = jnp.exp(jnp.log(3.0) * rise) * rough
    base = jnp.clip(jax.random.normal(key_base, (BATCH_SEQUENCES, D)), -5.0, 5.0)
    return (0.05 * base * scale[None, :]).astype(jnp.bfloat16)


def draw_key_cache(key, part):
    key_base = jax.random.fold_in(key, 0)
    result = jnp.clip(jax.random.normal(key_base, (BATCH_SEQUENCES, CACHE_LENGTH, KEY_VALUE_HEADS, HD)), -6.0, 6.0)
    return result.reshape(BATCH_SEQUENCES, CACHE_LENGTH, KEY_VALUE_HEADS * HD).astype(jnp.bfloat16)


def draw_decay_to_end(key, part):
    key_entries = jax.random.split(key, 7)
    slow_share = 0.5
    sluggish_flag = jax.random.uniform(key_entries[0], (KEY_VALUE_HEADS,)) < slow_share
    total = jnp.exp(jax.random.uniform(key_entries[1], (KEY_VALUE_HEADS,), minval=jnp.log(0.2), maxval=jnp.log(0.8)))
    fast_len = jnp.exp(jax.random.uniform(key_entries[2], (KEY_VALUE_HEADS,), minval=jnp.log(30.0), maxval=jnp.log(100.0)))
    mean_rate = jnp.where(sluggish_flag, total / CACHE_LENGTH, 1.0 / fast_len)
    shard_factor = jnp.exp(jax.random.uniform(key_entries[3], (BATCH_SEQUENCES, KEY_VALUE_HEADS, N_KV), minval=-0.7, maxval=0.7))
    block_of = jnp.arange(CACHE_LENGTH) // POS_DEV
    shard_pos = jnp.take(shard_factor, block_of, axis=2)
    rough = jnp.exp(jax.random.uniform(key_entries[4], (BATCH_SEQUENCES, KEY_VALUE_HEADS, CACHE_LENGTH), minval=jnp.log(0.3), maxval=jnp.log(3.0)))
    decode_steps = -mean_rate[None, :, None] * shard_pos * rough
    spike_offset = jax.random.randint(key_entries[5], (BATCH_SEQUENCES, KEY_VALUE_HEADS, 2), 0, CACHE_LENGTH)
    spike_length = jnp.log(jax.random.uniform(key_entries[6], (BATCH_SEQUENCES, KEY_VALUE_HEADS, 2), minval=0.55, maxval=0.8))
    decode_position = jnp.arange(CACHE_LENGTH)
    spike_count = jnp.where(decode_position[None, None, :] == spike_offset[:, :, 0:1], spike_length[:, :, 0:1], 0.0)
    spike_count = spike_count + jnp.where(decode_position[None, None, :] == spike_offset[:, :, 1:2], spike_length[:, :, 1:2], 0.0)
    decode_steps = decode_steps + jnp.where(sluggish_flag[None, :, None], spike_count, 0.0)
    later = jnp.cumsum(decode_steps[:, :, ::-1], axis=2)[:, :, ::-1] - decode_steps
    return later.astype(jnp.float32)


def steps_of(own_key, dims, shards, low, top_value):
    gain, own = 1.0, jax.random.fold_in(own_key, 6)
    for position, blocks in shards:
        heights = jnp.exp(jax.random.uniform(jax.random.fold_in(own, position), (blocks,), jnp.float32, low / len(shards), top_value / len(shards)))
        gain = gain * jnp.repeat(heights, dims[position] // blocks).reshape([-1 if axis == position else 1 for axis in range(len(dims))])
    return gain


def centred(key, dims, width, reach, cuts=(), kind=jnp.bfloat16):
    values = jax.random.normal(key, dims, jnp.float32) * width
    if len(cuts) > 0:
        values = steps_of(key, dims, cuts, -0.22, 0.18) * values
    return jnp.clip(values, min=-reach, max=reach).astype(kind)


def setup_inputs(seed: int = 0) -> dict:
    key_of = jax.random.split(jax.random.key(seed), 16)
    hidden_in = draw_hidden_in(jax.random.fold_in(key_of[15], 71), 0)
    pre_gain = jnp.clip(1.0 + 0.18 * jax.random.normal(key_of[1], (D,), jnp.float32), 0.1, 1.9)
    w_query = centred(key_of[2], (D, QH * HD), D ** -0.5, 0.09375, ((0, 16), (1, 8)))
    w_key = centred(key_of[3], (D, KEY_VALUE_HEADS * HD), D ** -0.5, 0.09375, ((0, 16), (1, 8)))
    w_value = centred(key_of[4], (D, KEY_VALUE_HEADS * HD), D ** -0.5, 0.09375, ((0, 16), (1, 8)))
    w_forget = centred(key_of[5], (D, KEY_VALUE_HEADS), D ** -0.5, 0.09375, ((0, 16),))
    forget_bias = jnp.clip(-2.0 + 3.5 * jax.random.uniform(key_of[6], (KEY_VALUE_HEADS,), jnp.float32) ** steps_of(key_of[6], (KEY_VALUE_HEADS,), ((0, 8),), -0.2, 0.2), -2.0, 1.5)
    key_cache = draw_key_cache(jax.random.fold_in(key_of[15], 71), 0)
    value_cache = centred(key_of[8], (BATCH_SEQUENCES, CACHE_LENGTH, KEY_VALUE_HEADS * HD), 1.0, 6.0, ((1, 16), (2, 8)))
    decay_to_end = draw_decay_to_end(jax.random.fold_in(key_of[15], 71), 0)
    w_output = centred(key_of[10], (QH * HD, D), (QH * HD) ** -0.5, 0.109375, ((0, 8), (1, 16)))
    mid_gain = jnp.clip(1.0 + 0.18 * jax.random.normal(key_of[11], (D,), jnp.float32), 0.1, 1.9)
    w_gate = centred(key_of[12], (D, FF), D ** -0.5, 0.09375, ((0, 16), (1, 8)))
    w_up = centred(key_of[13], (D, FF), D ** -0.5, 0.09375, ((0, 16), (1, 8)))
    w_down = centred(key_of[14], (FF, D), FF ** -0.5, 0.0546875, ((0, 8), (1, 16)))
    return {"hidden_in": hidden_in, "pre_gain": pre_gain, "w_query": w_query, "w_key": w_key, "w_value": w_value, "w_forget": w_forget, "forget_bias": forget_bias, "key_cache": key_cache, "value_cache": value_cache, "decay_to_end": decay_to_end, "w_output": w_output, "mid_gain": mid_gain, "w_gate": w_gate, "w_up": w_up, "w_down": w_down}


norm_eps = 1e-06

def grouped_sum(left, weight):
    groups = N_TP
    left_three = left.reshape(left.shape[0], groups, -1).astype(jnp.float32)
    weight_three = weight.reshape(groups, -1, weight.shape[1]).astype(jnp.float32)
    partial_terms = jnp.einsum('btk,tkd->btd', left_three, weight_three)
    rounded = lax.optimization_barrier(partial_terms.astype(jnp.bfloat16))
    return lax.optimization_barrier(jnp.sum(rounded.astype(jnp.float32), axis=1))

def attend_one(operands):
    query_b, keys_b, values_b, decay_b, key_own, value_own, log_b = operands
    score_scale = HD ** (-0.5)
    key_rows = keys_b.reshape(CACHE_LENGTH, KEY_VALUE_HEADS, HD).astype(jnp.float32)
    value_rows = values_b.reshape(CACHE_LENGTH, KEY_VALUE_HEADS, HD).astype(jnp.float32)
    query_f = query_b.astype(jnp.float32)
    scores = jnp.einsum('gqd,lgd->gql', query_f, key_rows) * score_scale
    scores = scores + log_b[:, None, None] + decay_b[:, None, :]
    own_score = jnp.einsum('gqd,gd->gq', query_f, key_own.astype(jnp.float32)) * score_scale
    largest = jnp.maximum(lax.optimization_barrier(jnp.max(scores, axis=2)), own_score)
    weights = jnp.exp(scores - largest[:, :, None])
    own_weight = jnp.exp(own_score - largest)
    total = lax.optimization_barrier(jnp.sum(weights, axis=2)) + own_weight
    rounded = lax.optimization_barrier(weights.astype(jnp.bfloat16))
    mixed = jnp.einsum('gql,lgd->gqd', rounded.astype(jnp.float32), value_rows)
    mixed = mixed + own_weight[:, :, None] * value_own.astype(jnp.float32)[:, None, :]
    return mixed / total[:, :, None]

def reference(hidden_in, pre_gain, w_query, w_key, w_value, w_forget, forget_bias, key_cache, value_cache, decay_to_end, w_output, mid_gain, w_gate, w_up, w_down):
    group_size = QH // KEY_VALUE_HEADS
    x_float = hidden_in.astype(jnp.float32)
    inv_rms = lax.rsqrt(lax.optimization_barrier(jnp.mean(x_float * x_float, axis=1, keepdims=True)) + norm_eps)
    scaled = (x_float * pre_gain).astype(jnp.bfloat16)
    query = (jnp.dot(scaled, w_query, preferred_element_type=jnp.float32) * inv_rms).astype(jnp.bfloat16)
    key_new = (jnp.dot(scaled, w_key, preferred_element_type=jnp.float32) * inv_rms).astype(jnp.bfloat16)
    value_new = (jnp.dot(scaled, w_value, preferred_element_type=jnp.float32) * inv_rms).astype(jnp.bfloat16)
    log_new = jax.nn.log_sigmoid(jnp.dot(scaled, w_forget, preferred_element_type=jnp.float32) * inv_rms + forget_bias)
    attended = lax.map(attend_one, (query.reshape(BATCH_SEQUENCES, KEY_VALUE_HEADS, group_size, HD), key_cache, value_cache, decay_to_end, key_new.reshape(BATCH_SEQUENCES, KEY_VALUE_HEADS, HD), value_new.reshape(BATCH_SEQUENCES, KEY_VALUE_HEADS, HD), log_new))
    attended = attended.reshape(BATCH_SEQUENCES, QH * HD).astype(jnp.bfloat16)
    projected = grouped_sum(attended, w_output)
    mid_float = x_float + projected
    mid_inv = lax.rsqrt(lax.optimization_barrier(jnp.mean(mid_float * mid_float, axis=1, keepdims=True)) + norm_eps)
    mid_scaled = (mid_float * mid_gain).astype(jnp.bfloat16)
    gate = jnp.dot(mid_scaled, w_gate, preferred_element_type=jnp.float32) * mid_inv
    upward = jnp.dot(mid_scaled, w_up, preferred_element_type=jnp.float32) * mid_inv
    hidden_units = (jax.nn.silu(gate) * upward).astype(jnp.bfloat16)
    lowered = grouped_sum(hidden_units, w_down)
    return mid_float + lowered
```

```python
import functools

import jax
import jax.numpy as jnp
from jax import lax
from jax.experimental import pallas as pl
from jax.experimental.pallas import tpu as pltpu
from jax.sharding import PartitionSpec as P

D = 4096
QH = 48
KEY_VALUE_HEADS = 16
HD = 64
NORM_EPS = 1e-06
MESH = pl.DeviceIdType.MESH
F32 = jnp.float32
BF16 = jnp.bfloat16


def kernel(
    n_kv,
    n_tp,
    hidden_in,
    pre_gain,
    w_query,
    w_key,
    w_value,
    w_forget,
    forget_bias,
    key_cache,
    value_cache,
    decay,
    w_output,
    mid_gain,
    w_gate,
    w_up,
    w_down,
    out_ref,
    xs,
    pg,
    wq,
    wk,
    wv,
    wf,
    fb,
    kc,
    vc,
    dec,
    wo,
    mg,
    wg,
    wu,
    wd,
    load_sem,
    dec_rows,
    q_mine,
    q_in,
    s_mine,
    s_in,
    t_mine,
    t_in,
    q_rows,
    o_rows,
    l_rows,
    a_mine,
    a_in,
    e_mine,
    e_in,
    p_mine,
    p_in,
    g_rows,
    g_mine,
    g_in,
    h_all,
    h_rows,
    d_mine,
    d_in,
    x_send,
    x_recv,
    q_send,
    q_recv,
    s_send,
    s_recv,
    t_send,
    t_recv,
    a_send,
    a_recv,
    e_send,
    e_recv,
    p_send,
    p_recv,
    g_send,
    g_recv,
    h_send,
    h_recv,
    d_send,
    d_recv,
):
    kv = lax.axis_index("kv")
    tp = lax.axis_index("tp")
    kv_peers = [lax.rem(kv + d, n_kv) for d in range(1, n_kv)]
    tp_peers = [lax.rem(tp + d, n_tp) for d in range(1, n_tp)]

    loads = [
        (hidden_in, xs.at[tp]),
        (pre_gain, pg),
        (w_query, wq),
        (w_key, wk),
        (w_value, wv),
        (w_forget, wf),
        (forget_bias, fb),
        (decay, dec),
        (key_cache, kc),
        (value_cache, vc),
        (w_output, wo),
        (mid_gain, mg),
        (w_gate, wg),
        (w_up, wu),
        (w_down, wd),
    ]
    loads = [pltpu.make_async_copy(a, b, load_sem.at[i]) for i, (a, b) in enumerate(loads)]
    for copy in loads:
        copy.start()
    (l_x, l_pg, l_wq, l_wk, l_wv, l_wf, l_fb, l_dec, l_kc, l_vc, l_wo, l_mg, l_wg, l_wu, l_wd) = loads

    barrier = pltpu.get_barrier_semaphore()
    for peer in kv_peers:
        pl.semaphore_signal(barrier, inc=1, device_id={"kv": peer, "tp": tp}, device_id_type=MESH)
    for peer in tp_peers:
        pl.semaphore_signal(barrier, inc=1, device_id={"kv": kv, "tp": peer}, device_id_type=MESH)
    pl.semaphore_wait(barrier, n_kv + n_tp - 2)

    def send(axis, src, dst, send_sem, recv_sem):
        peers = kv_peers if axis == "kv" else tp_peers
        copies = []
        for i, peer in enumerate(peers):
            device = {"kv": peer, "tp": tp} if axis == "kv" else {"kv": kv, "tp": peer}
            copy = pltpu.make_async_remote_copy(
                src_ref=src(peer),
                dst_ref=dst(i),
                send_sem=send_sem.at[i],
                recv_sem=recv_sem.at[i],
                device_id=device,
                device_id_type=MESH,
            )
            copy.start()
            copies.append(copy)
        return copies

    def received(copies):
        for copy in copies:
            copy.wait_recv()

    def sent(copies):
        for copy in copies:
            copy.wait_send()

    lane = lax.broadcasted_iota(jnp.int32, (16, 128), 1)
    low = lane < 64

    l_x.wait()
    x_copies = send("tp", lambda peer: xs.at[tp], lambda i: xs.at[tp], x_send, x_recv)

    q_rows[...] = jnp.zeros_like(q_rows)
    l_dec.wait()
    row = lax.broadcasted_iota(jnp.int32, (8, 1024), 0)
    for b in range(16):
        dec_rows[b] = jnp.where(row < 3, dec[b, 0:1, :], dec[b, 1:2, :])
    for copy in (l_pg, l_wq, l_wk, l_wv, l_wf, l_fb):
        copy.wait()

    received(x_copies)
    x = jnp.concatenate([xs[t].astype(F32) for t in range(n_tp)], axis=1)
    scaled = (x * pg[...]).astype(BF16)
    q_part = jnp.dot(scaled, wq[...], preferred_element_type=F32)
    q_mine[...] = q_part
    square = jnp.sum(x * x, axis=1, keepdims=True)
    square = jnp.broadcast_to(square, (16, 128))
    s_mine[...] = jnp.where(low[0:8], square[0:8], square[8:16])
    q_copies = send("kv", lambda peer: q_mine, lambda i: q_in.at[i], q_send, q_recv)
    s_copies = send("kv", lambda peer: s_mine, lambda i: s_in.at[i], s_send, s_recv)

    k_part = jnp.dot(scaled, wk[...], preferred_element_type=F32)
    v_part = jnp.dot(scaled, wv[...], preferred_element_type=F32)
    f_part = jnp.dot(scaled, wf[...], preferred_element_type=F32)
    f_col = lax.broadcasted_iota(jnp.int32, (16, 16), 1)
    f_zero = jnp.zeros_like(f_part)
    f_first = jnp.sum(jnp.where(f_col == 2 * tp, f_part, f_zero), axis=1, keepdims=True)
    f_second = jnp.sum(jnp.where(f_col == 2 * tp + 1, f_part, f_zero), axis=1, keepdims=True)
    f_wide = jnp.where(low, f_first, f_second)
    t_mine[pl.ds(0, 16, stride=8), :] = k_part
    t_mine[pl.ds(1, 16, stride=8), :] = v_part
    t_mine[pl.ds(2, 16, stride=8), :] = f_wide
    t_mine[pl.ds(3, 16, stride=8), :] = square
    t_copies = send(
        "kv", lambda peer: t_mine.at[pl.ds(pl.multiple_of(peer * 8, 8), 8)], lambda i: t_in.at[i], t_send, t_recv
    )
    sent(x_copies)
    l_kc.wait()
    l_vc.wait()

    received(q_copies)
    received(s_copies)
    q_sum = q_mine[...]
    s_sum = s_mine[...]
    for i in range(n_kv - 1):
        q_sum = q_sum + q_in[i]
        s_sum = s_sum + s_in[i]
    s_sum = jnp.concatenate([s_sum[:, 0:1], s_sum[:, 64:65]], axis=0)
    inv_rms = lax.rsqrt(s_sum / D + NORM_EPS)
    query = (q_sum * inv_rms).astype(BF16).astype(F32) * (HD**-0.5)
    zero = jnp.zeros((16, 128), F32)
    for h in range(6):
        c, half, g = h // 2, h % 2, h // 3
        part = query[:, c * 128 : (c + 1) * 128]
        if half != g:
            part = pltpu.roll(part, 64, 1)
        q_rows[pl.ds(h, 16, stride=8), :] = jnp.where(low if g == 0 else ~low, part, zero)

    received(t_copies)
    t_sum = t_mine[pl.ds(pl.multiple_of(kv * 8, 8), 8), :]
    for i in range(n_kv - 1):
        t_sum = t_sum + t_in[i]
    t_inv = lax.rsqrt(t_sum[3:4, :] / D + NORM_EPS)
    key_new = (t_sum[0:1, :] * t_inv).astype(BF16).astype(F32)
    value_new = (t_sum[1:2, :] * t_inv).astype(BF16).astype(F32)
    low8 = low[0:8]
    row8 = lax.broadcasted_iota(jnp.int32, (8, 128), 0)
    gate_in = t_sum[2:3, :] * t_inv + jnp.where(low[0:1], fb[0:1, 0:1], fb[0:1, 1:2])
    log_new = jnp.minimum(gate_in, 0.0) - jnp.log1p(jnp.exp(-jnp.abs(gate_in)))
    q_own = q_rows[pl.ds(pl.multiple_of(kv * 8, 8), 8), :]
    own = jnp.sum(q_own * key_new, axis=1, keepdims=True)
    own = own - jnp.where(row8[:, 0:1] < 3, log_new[:, 0:1], log_new[:, 64:65])

    for b in range(16):
        q8 = q_rows[b * 8 : (b + 1) * 8, :].astype(BF16)
        scores = lax.dot_general(q8, kc[b], (((1,), (1,)), ((), ())), preferred_element_type=F32)
        scores = scores + dec_rows[b]
        own_b = jnp.where(kv == b, own, -jnp.inf)
        top = jnp.maximum(jnp.max(scores, axis=1, keepdims=True), own_b)
        weights = jnp.exp(scores - top)
        own_weight = jnp.exp(own_b - top)
        total = jnp.sum(weights, axis=1, keepdims=True) + own_weight
        mixed = jnp.dot(weights.astype(BF16), vc[b], preferred_element_type=F32)
        mixed = mixed + own_weight * value_new
        o_rows[b * 8 : (b + 1) * 8, :] = mixed / total
        l_rows[b * 8 : (b + 1) * 8, :] = jnp.broadcast_to(top + jnp.log(total), (8, 128))

    heads = [o_rows[pl.ds(h, 16, stride=8), :] for h in range(6)]
    logs = [l_rows[pl.ds(h, 16, stride=8), :] for h in range(6)]
    chunk_0 = jnp.where(low, heads[0], pltpu.roll(heads[1], 64, 1))
    chunk_1 = jnp.where(low, heads[2], heads[3])
    chunk_2 = jnp.where(low, pltpu.roll(heads[4], 64, 1), heads[5])
    mine = jnp.concatenate([chunk_0, chunk_1, chunk_2], axis=1).astype(BF16)
    a_mine[...] = mine
    e_wide = logs[0]
    for h in range(1, 6):
        e_wide = jnp.where(lane < 16 * h, e_wide, logs[h])
    e_mine[...] = e_wide
    e_copies = send("kv", lambda peer: e_mine, lambda i: e_in.at[i], e_send, e_recv)
    a_copies = send("kv", lambda peer: a_mine, lambda i: a_in.at[i], a_send, a_recv)
    sent(q_copies)
    sent(s_copies)
    sent(t_copies)
    received(e_copies)
    parts = [e_wide] + [e_in[i] for i in range(n_kv - 1)]
    top = functools.reduce(jnp.maximum, parts)
    shares = [jnp.exp(part - top) for part in parts]
    whole = functools.reduce(jnp.add, shares)
    inverse = 1.0 / whole
    l_wo.wait()
    received(a_copies)
    attended = jnp.zeros((16, 384), F32)
    for i in range(n_kv):
        share = shares[i] * inverse
        wide = jnp.concatenate(
            [jnp.broadcast_to(share[:, 16 * h : 16 * h + 1], (16, 128)) for h in range(6)], axis=1
        )
        wide = jnp.concatenate(
            [
                jnp.where(low, wide[:, 256 * c : 256 * c + 128], wide[:, 256 * c + 128 : 256 * c + 256])
                for c in range(3)
            ],
            axis=1,
        )
        value = mine if i == 0 else a_in[i - 1]
        attended = attended + wide * value.astype(F32)

    part = jnp.dot(attended.astype(BF16), wo[...], preferred_element_type=F32).astype(BF16)
    p_mine[...] = part
    p_copies = send("tp", lambda peer: p_mine, lambda i: p_in.at[i], p_send, p_recv)
    sent(e_copies)
    sent(a_copies)
    for copy in (l_mg, l_wg, l_wu, l_wd):
        copy.wait()
    received(p_copies)
    projected = part.astype(F32)
    for i in range(n_tp - 1):
        projected = projected + p_in[i].astype(F32)
    mid = x + projected
    mid_scaled = (mid * mg[...]).astype(BF16)
    gate_part = jnp.dot(mid_scaled, wg[...], preferred_element_type=F32)
    up_part = jnp.dot(mid_scaled, wu[...], preferred_element_type=F32)
    mid_square = jnp.broadcast_to(jnp.sum(mid * mid, axis=1, keepdims=True), (16, 128))
    square_high = mid_square.astype(BF16).astype(F32)
    for c in range(11):
        g_rows[pl.ds(c, 16, stride=24), :] = gate_part[:, 128 * c : 128 * (c + 1)]
        g_rows[pl.ds(11 + c, 16, stride=24), :] = up_part[:, 128 * c : 128 * (c + 1)]
    g_rows[pl.ds(22, 16, stride=24), :] = square_high
    g_rows[pl.ds(23, 16, stride=24), :] = mid_square - square_high
    for b in range(16):
        g_mine[b] = g_rows[24 * b : 24 * (b + 1), :].astype(BF16)
    g_copies = send("kv", lambda peer: g_mine.at[peer], lambda i: g_in.at[i], g_send, g_recv)
    sent(p_copies)
    received(g_copies)
    g_sum = g_mine[kv].astype(F32)
    for i in range(n_kv - 1):
        g_sum = g_sum + g_in[i].astype(F32)
    mid_inv = lax.rsqrt((g_sum[22:23, :] + g_sum[23:24, :]) / D + NORM_EPS)
    gate = g_sum[0:11, :] * mid_inv
    up = g_sum[11:22, :] * mid_inv
    hidden = gate / (1.0 + jnp.exp(-gate)) * up
    hidden = jnp.concatenate([hidden, jnp.zeros((5, 128), F32)], axis=0).astype(BF16)
    h_all[kv] = hidden
    h_copies = send("kv", lambda peer: h_all.at[kv], lambda i: h_all.at[kv], h_send, h_recv)
    sent(g_copies)
    received(h_copies)
    for b in range(16):
        h_rows[16 * b : 16 * (b + 1), :] = h_all[b].astype(F32)
    units = jnp.concatenate([h_rows[pl.ds(c, 16, stride=16), :] for c in range(11)], axis=1).astype(BF16)
    down = jnp.dot(units, wd[...], preferred_element_type=F32).astype(BF16)
    d_mine[0] = down[:, 0:128]
    d_mine[1] = down[:, 128:256]
    d_copies = send("tp", lambda peer: d_mine.at[peer // 4], lambda i: d_in.at[i], d_send, d_recv)
    sent(h_copies)
    result = d_mine[tp // 4].astype(F32)
    received(d_copies)
    for i in range(n_tp - 1):
        result = result + d_in[i].astype(F32)
    result = jnp.where(tp < 4, mid[:, 0:128], mid[:, 128:256]) + result
    place = lax.rem(tp, 4)
    pick = result[:, 0:32]
    for r in range(1, 4):
        pick = jnp.where(place == r, result[:, 32 * r : 32 * (r + 1)], pick)
    out_ref[...] = pick
    sent(d_copies)


def on_device(n_kv, n_tp, *args):
    args = list(args)
    for i in (1, 6, 11):
        args[i] = args[i].reshape(1, -1)
    vmem = pltpu.VMEM
    own = [vmem(a.shape, a.dtype) for a in args[1:]]
    kv_other, tp_other = n_kv - 1, n_tp - 1
    dma = pltpu.SemaphoreType.DMA
    scratch = [
        vmem((n_tp, 16, 32), BF16),
        *own,
        dma((15,)),
        vmem((16, 8, 1024), F32),
        vmem((16, 384), F32),
        vmem((kv_other, 16, 384), F32),
        vmem((8, 128), F32),
        vmem((kv_other, 8, 128), F32),
        vmem((128, 128), F32),
        vmem((kv_other, 8, 128), F32),
        vmem((128, 128), F32),
        vmem((128, 128), F32),
        vmem((128, 128), F32),
        vmem((16, 384), BF16),
        vmem((kv_other, 16, 384), BF16),
        vmem((16, 128), F32),
        vmem((kv_other, 16, 128), F32),
        vmem((16, 256), BF16),
        vmem((tp_other, 16, 256), BF16),
        vmem((16 * 24, 128), F32),
        vmem((16, 24, 128), BF16),
        vmem((kv_other, 24, 128), BF16),
        vmem((16, 16, 128), BF16),
        vmem((256, 128), F32),
        vmem((2, 16, 128), BF16),
        vmem((tp_other, 16, 128), BF16),
    ]
    for n in (tp_other, kv_other, kv_other, kv_other, kv_other, kv_other, tp_other, kv_other, kv_other, tp_other):
        scratch += [dma((n,)), dma((n,))]
    return pl.pallas_call(
        functools.partial(kernel, n_kv, n_tp),
        out_shape=jax.ShapeDtypeStruct((16, 32), F32),
        in_specs=[pl.BlockSpec(memory_space=pl.ANY)] * len(args),
        out_specs=pl.BlockSpec(memory_space=pltpu.VMEM),
        scratch_shapes=scratch,
        compiler_params=pltpu.CompilerParams(
            collective_id=0, has_side_effects=True, vmem_limit_bytes=60 * 1024 * 1024
        ),
        name="layer_step",
    )(*args)


def solution(mesh):
    return jax.shard_map(
        functools.partial(on_device, mesh.shape["kv"], mesh.shape["tp"]),
        mesh=mesh,
        in_specs=(
            P(None, ("kv", "tp")),
            P("kv"),
            P("kv", "tp"),
            P("kv", "tp"),
            P("kv", "tp"),
            P("kv", None),
            P("tp"),
            P(None, "kv", "tp"),
            P(None, "kv", "tp"),
            P(None, "tp", "kv"),
            P("tp", "kv"),
            P("kv"),
            P("kv", "tp"),
            P("kv", "tp"),
            P("tp", "kv"),
        ),
        out_specs=P(None, ("kv", "tp")),
        check_vma=False,
    )
```

```python
import functools

import jax
import jax.numpy as jnp
from jax import lax
from jax.experimental import pallas as pl
from jax.experimental.pallas import tpu as pltpu
from jax.sharding import PartitionSpec as P

D = 4096
QH = 48
KEY_VALUE_HEADS = 16
HD = 64
NORM_EPS = 1e-06
MESH = pl.DeviceIdType.MESH
F32 = jnp.float32
BF16 = jnp.bfloat16


def kernel(
    n_kv,
    n_tp,
    hidden_in,
    pre_gain,
    w_query,
    w_key,
    w_value,
    w_forget,
    forget_bias,
    key_cache,
    value_cache,
    decay,
    w_output,
    mid_gain,
    w_gate,
    w_up,
    w_down,
    out_ref,
    xs,
    pg,
    wq,
    wk,
    wv,
    wf,
    fb,
    kc,
    vc,
    dec,
    wo,
    mg,
    wg,
    wu,
    wd,
    load_sem,
    plane,
    dec_rows,
    q_mine,
    q_in,
    s_mine,
    s_in,
    t_mine,
    t_in,
    q_rows,
    o_rows,
    l_rows,
    own_rows,
    top_rows,
    sum_rows,
    a_mine,
    a_in,
    e_mine,
    e_in,
    p_mine,
    p_in,
    g_rows,
    g_mine,
    g_in,
    h_all,
    h_rows,
    d_mine,
    d_in,
    x_send,
    x_recv,
    q_send,
    q_recv,
    s_send,
    s_recv,
    t_send,
    t_recv,
    a_send,
    a_recv,
    e_send,
    e_recv,
    p_send,
    p_recv,
    g_send,
    g_recv,
    h_send,
    h_recv,
    d_send,
    d_recv,
):
    kv = lax.axis_index("kv")
    tp = lax.axis_index("tp")
    kv_peers = [lax.rem(kv + d, n_kv) for d in range(1, n_kv)]
    tp_peers = [lax.rem(tp + d, n_tp) for d in range(1, n_tp)]

    side = 4
    z_line = [lax.rem(kv + side * d, n_kv) for d in range(1, n_kv // side)]
    x_line = [kv // side * side + lax.rem(kv + d, side) for d in range(1, side)]
    barrier = pltpu.get_barrier_semaphore()
    for peer in tp_peers:
        pl.semaphore_signal(barrier, inc=1, device_id={"kv": kv, "tp": peer}, device_id_type=MESH)
    for peer in z_line + x_line:
        pl.semaphore_signal(barrier, inc=1, device_id={"kv": peer, "tp": tp}, device_id_type=MESH)

    loads = [
        (hidden_in, xs.at[tp]),
        (pre_gain, pg),
        (w_query, wq),
        (w_key, wk),
        (w_value, wv),
        (w_forget, wf),
        (forget_bias, fb),
        (decay, dec),
        (key_cache, kc),
        (value_cache, vc),
        (w_output, wo),
        (mid_gain, mg),
        (w_gate, wg),
        (w_up, wu),
        (w_down, wd),
    ]
    loads = [pltpu.make_async_copy(a, b, load_sem.at[i]) for i, (a, b) in enumerate(loads)]
    for copy in loads:
        copy.start()
    (l_x, l_pg, l_wq, l_wk, l_wv, l_wf, l_fb, l_dec, l_kc, l_vc, l_wo, l_mg, l_wg, l_wu, l_wd) = loads

    def send(axis, src, dst, landed, send_sem, recv_sem):
        peers = kv_peers if axis == "kv" else tp_peers
        for i, peer in enumerate(peers):
            device = {"kv": peer, "tp": tp} if axis == "kv" else {"kv": kv, "tp": peer}
            pltpu.make_async_remote_copy(
                src_ref=src(peer),
                dst_ref=dst(i),
                send_sem=send_sem,
                recv_sem=recv_sem,
                device_id=device,
                device_id_type=MESH,
            ).start()
        return pltpu.make_async_remote_copy(
            src_ref=landed,
            dst_ref=landed,
            send_sem=send_sem,
            recv_sem=recv_sem,
            device_id=device,
            device_id_type=MESH,
        )

    def received(copy):
        copy.wait_recv()

    def sent(copy):
        copy.wait_send()

    lane = lax.broadcasted_iota(jnp.int32, (16, 128), 1)
    low = lane < 64

    pl.semaphore_wait(barrier, n_tp - 1 + len(z_line) + len(x_line))
    for peer in x_line:
        pl.semaphore_signal(plane, inc=1, device_id={"kv": peer, "tp": tp}, device_id_type=MESH)
    l_x.wait()
    x_copies = send("tp", lambda peer: xs.at[tp], lambda i: xs.at[tp], xs.at[pl.ds(0, n_tp - 1)], x_send, x_recv)

    q_rows[...] = jnp.zeros_like(q_rows)
    l_dec.wait()
    row = lax.broadcasted_iota(jnp.int32, (8, 1024), 0)
    for b in range(16):
        dec_rows[b] = jnp.where(row < 3, dec[b, 0:1, :], dec[b, 1:2, :])
    for copy in (l_pg, l_wq, l_wk, l_wv, l_wf, l_fb):
        copy.wait()

    received(x_copies)
    x = jnp.concatenate([xs[t].astype(F32) for t in range(n_tp)], axis=1)
    scaled = (x * pg[...]).astype(BF16)
    q_part = jnp.dot(scaled, wq[...], preferred_element_type=F32)
    q_mine[...] = q_part
    square = jnp.sum(x * x, axis=1, keepdims=True)
    square = jnp.broadcast_to(square, (16, 128))
    s_mine[...] = jnp.where(low[0:8], square[0:8], square[8:16])
    pl.semaphore_wait(plane, len(x_line))
    q_copies = send("kv", lambda peer: q_mine, lambda i: q_in.at[i], q_in, q_send, q_recv)
    s_copies = send("kv", lambda peer: s_mine, lambda i: s_in.at[i], s_in, s_send, s_recv)

    k_part = jnp.dot(scaled, wk[...], preferred_element_type=F32)
    v_part = jnp.dot(scaled, wv[...], preferred_element_type=F32)
    f_part = lax.dot_general(scaled, wf[...], (((1,), (1,)), ((), ())), preferred_element_type=F32)
    f_col = lax.broadcasted_iota(jnp.int32, (16, 16), 1)
    f_zero = jnp.zeros_like(f_part)
    f_first = jnp.sum(jnp.where(f_col == 2 * tp, f_part, f_zero), axis=1, keepdims=True)
    f_second = jnp.sum(jnp.where(f_col == 2 * tp + 1, f_part, f_zero), axis=1, keepdims=True)
    f_wide = jnp.where(low, f_first, f_second)
    t_mine[pl.ds(0, 16, stride=8), :] = k_part
    t_mine[pl.ds(1, 16, stride=8), :] = v_part
    t_mine[pl.ds(2, 16, stride=8), :] = f_wide
    t_mine[pl.ds(3, 16, stride=8), :] = square
    t_copies = send(
        "kv", lambda peer: t_mine.at[pl.ds(pl.multiple_of(peer * 8, 8), 8)], lambda i: t_in.at[i], t_in, t_send, t_recv
    )
    sent(x_copies)
    l_kc.wait()
    l_vc.wait()

    received(q_copies)
    received(s_copies)
    q_sum = q_mine[...]
    s_sum = s_mine[...]
    for i in range(n_kv - 1):
        q_sum = q_sum + q_in[i]
        s_sum = s_sum + s_in[i]
    s_sum = jnp.concatenate([s_sum[:, 0:1], s_sum[:, 64:65]], axis=0)
    inv_rms = lax.rsqrt(s_sum / D + NORM_EPS)
    query = (q_sum * inv_rms).astype(BF16).astype(F32) * (HD**-0.5)
    zero = jnp.zeros((16, 128), F32)
    for h in range(6):
        c, half, g = h // 2, h % 2, h // 3
        part = query[:, c * 128 : (c + 1) * 128]
        if half != g:
            part = pltpu.roll(part, 64, 1)
        q_rows[pl.ds(h, 16, stride=8), :] = jnp.where(low if g == 0 else ~low, part, zero)

    received(t_copies)
    t_sum = t_mine[pl.ds(pl.multiple_of(kv * 8, 8), 8), :]
    for i in range(n_kv - 1):
        t_sum = t_sum + t_in[i]
    t_inv = lax.rsqrt(t_sum[3:4, :] / D + NORM_EPS)
    key_new = (t_sum[0:1, :] * t_inv).astype(BF16).astype(F32)
    value_new = (t_sum[1:2, :] * t_inv).astype(BF16).astype(F32)
    low8 = low[0:8]
    row8 = lax.broadcasted_iota(jnp.int32, (8, 128), 0)
    gate_in = t_sum[2:3, :] * t_inv + jnp.where(low[0:1], fb[0:1, 0:1], fb[0:1, 1:2])
    log_new = jnp.minimum(gate_in, 0.0) - jnp.log1p(jnp.exp(-jnp.abs(gate_in)))
    q_own = q_rows[pl.ds(pl.multiple_of(kv * 8, 8), 8), :]
    own = jnp.sum(q_own * key_new, axis=1, keepdims=True)
    own = own - jnp.where(row8[:, 0:1] < 3, log_new[:, 0:1], log_new[:, 64:65])

    own_here = jnp.broadcast_to(own, (8, 128))
    absent = jnp.full((8, 128), -jnp.inf, F32)
    for b in range(16):
        own_rows[8 * b : 8 * (b + 1), :] = jnp.where(kv == b, own_here, absent)
    for b in range(16):
        q8 = q_rows[8 * b : 8 * (b + 1), :].astype(BF16)
        scores = lax.dot_general(q8, kc[b], (((1,), (1,)), ((), ())), preferred_element_type=F32)
        scores = scores + dec_rows[b]
        top_rows[8 * b : 8 * (b + 1), :] = functools.reduce(
            jnp.maximum, [scores[:, 128 * j : 128 * (j + 1)] for j in range(8)]
        )
        dec_rows[b] = scores
    own_all = own_rows[...]
    top = jnp.maximum(jnp.max(top_rows[...], axis=1, keepdims=True), own_all)
    top_rows[...] = top
    for b in range(16):
        top_b = top_rows[8 * b : 8 * (b + 1), :]
        weights = jnp.exp(dec_rows[b] - jnp.concatenate([top_b] * 8, axis=1))
        sum_rows[8 * b : 8 * (b + 1), :] = functools.reduce(
            jnp.add, [weights[:, 128 * j : 128 * (j + 1)] for j in range(8)]
        )
        o_rows[8 * b : 8 * (b + 1), :] = jnp.dot(weights.astype(BF16), vc[b], preferred_element_type=F32)
    own_weight = jnp.exp(own_all - top)
    total = jnp.sum(sum_rows[...], axis=1, keepdims=True) + own_weight
    o_rows[...] = (o_rows[...] + own_weight * value_new) / total
    l_rows[...] = top + jnp.log(total)

    heads = [o_rows[pl.ds(h, 16, stride=8), :] for h in range(6)]
    logs = [l_rows[pl.ds(h, 16, stride=8), :] for h in range(6)]
    chunk_0 = jnp.where(low, heads[0], pltpu.roll(heads[1], 64, 1))
    chunk_1 = jnp.where(low, heads[2], heads[3])
    chunk_2 = jnp.where(low, pltpu.roll(heads[4], 64, 1), heads[5])
    mine = jnp.concatenate([chunk_0, chunk_1, chunk_2], axis=1).astype(BF16)
    a_mine[...] = mine
    spot = lax.rem(lane, 64)
    e_wide = logs[0]
    for h in range(1, 6):
        e_wide = jnp.where(spot < 8 * h, e_wide, logs[h])
    e_wide = jnp.where(low[0:8], e_wide[0:8], e_wide[8:16])
    e_mine[...] = e_wide
    e_copies = send("kv", lambda peer: e_mine, lambda i: e_in.at[i], e_in, e_send, e_recv)
    a_copies = send("kv", lambda peer: a_mine, lambda i: a_in.at[i], a_in, a_send, a_recv)
    sent(q_copies)
    sent(s_copies)
    sent(t_copies)
    received(e_copies)
    parts = [e_wide] + [e_in[i] for i in range(n_kv - 1)]
    top = functools.reduce(jnp.maximum, parts)
    shares = [jnp.exp(part - top) for part in parts]
    whole = functools.reduce(jnp.add, shares)
    inverse = 1.0 / whole
    l_wo.wait()
    received(a_copies)
    attended = jnp.zeros((16, 384), F32)
    for i in range(n_kv):
        share = shares[i] * inverse
        wide = [
            jnp.concatenate([jnp.broadcast_to(share[:, at : at + 1], (8, 128)) for at in (8 * h, 64 + 8 * h)], axis=0)
            for h in range(6)
        ]
        wide = jnp.concatenate([jnp.where(low, wide[2 * c], wide[2 * c + 1]) for c in range(3)], axis=1)
        value = mine if i == 0 else a_in[i - 1]
        attended = attended + wide * value.astype(F32)

    part = jnp.dot(attended.astype(BF16), wo[...], preferred_element_type=F32).astype(BF16)
    p_mine[...] = part
    p_copies = send("tp", lambda peer: p_mine, lambda i: p_in.at[i], p_in, p_send, p_recv)
    sent(e_copies)
    sent(a_copies)
    for copy in (l_mg, l_wg, l_wu, l_wd):
        copy.wait()
    received(p_copies)
    projected = part.astype(F32)
    for i in range(n_tp - 1):
        projected = projected + p_in[i].astype(F32)
    mid = x + projected
    mid_scaled = (mid * mg[...]).astype(BF16)
    gate_part = jnp.dot(mid_scaled, wg[...], preferred_element_type=F32)
    up_part = jnp.dot(mid_scaled, wu[...], preferred_element_type=F32)
    mid_square = jnp.broadcast_to(jnp.sum(mid * mid, axis=1, keepdims=True), (16, 128))
    square_high = mid_square.astype(BF16).astype(F32)
    for c in range(11):
        g_rows[pl.ds(c, 16, stride=24), :] = gate_part[:, 128 * c : 128 * (c + 1)]
        g_rows[pl.ds(11 + c, 16, stride=24), :] = up_part[:, 128 * c : 128 * (c + 1)]
    g_rows[pl.ds(22, 16, stride=24), :] = square_high
    g_rows[pl.ds(23, 16, stride=24), :] = mid_square - square_high
    for b in range(16):
        g_mine[b] = g_rows[24 * b : 24 * (b + 1), :].astype(BF16)
    g_copies = send("kv", lambda peer: g_mine.at[peer], lambda i: g_in.at[i], g_in, g_send, g_recv)
    sent(p_copies)
    received(g_copies)
    g_sum = g_mine[kv].astype(F32)
    for i in range(n_kv - 1):
        g_sum = g_sum + g_in[i].astype(F32)
    mid_inv = lax.rsqrt((g_sum[22:23, :] + g_sum[23:24, :]) / D + NORM_EPS)
    gate = g_sum[0:11, :] * mid_inv
    up = g_sum[11:22, :] * mid_inv
    hidden = gate / (1.0 + jnp.exp(-gate)) * up
    hidden = jnp.concatenate([hidden, jnp.zeros((5, 128), F32)], axis=0).astype(BF16)
    h_all[kv] = hidden
    h_copies = send("kv", lambda peer: h_all.at[kv], lambda i: h_all.at[kv], h_all.at[pl.ds(0, n_kv - 1)], h_send, h_recv)
    sent(g_copies)
    received(h_copies)
    for b in range(16):
        h_rows[16 * b : 16 * (b + 1), :] = h_all[b].astype(F32)
    units = jnp.concatenate([h_rows[pl.ds(c, 16, stride=16), :] for c in range(11)], axis=1).astype(BF16)
    down = jnp.dot(units, wd[...], preferred_element_type=F32).astype(BF16)
    d_mine[0] = down[:, 0:128]
    d_mine[1] = down[:, 128:256]
    d_copies = send("tp", lambda peer: d_mine.at[peer // 4], lambda i: d_in.at[i], d_in, d_send, d_recv)
    sent(h_copies)
    result = d_mine[tp // 4].astype(F32)
    received(d_copies)
    for i in range(n_tp - 1):
        result = result + d_in[i].astype(F32)
    result = jnp.where(tp < 4, mid[:, 0:128], mid[:, 128:256]) + result
    place = lax.rem(tp, 4)
    pick = result[:, 0:32]
    for r in range(1, 4):
        pick = jnp.where(place == r, result[:, 32 * r : 32 * (r + 1)], pick)
    out_ref[...] = pick
    sent(d_copies)


def on_device(n_kv, n_tp, *args):
    args = list(args)
    for i in (1, 6, 11):
        args[i] = args[i].reshape(1, -1)
    args[5] = args[5].T
    vmem = pltpu.VMEM
    own = [vmem(a.shape, a.dtype) for a in args[1:]]
    kv_other, tp_other = n_kv - 1, n_tp - 1
    dma = pltpu.SemaphoreType.DMA
    scratch = [
        vmem((n_tp, 16, 32), BF16),
        *own,
        dma((15,)),
        pltpu.SemaphoreType.REGULAR,
        vmem((16, 8, 1024), F32),
        vmem((16, 384), F32),
        vmem((kv_other, 16, 384), F32),
        vmem((8, 128), F32),
        vmem((kv_other, 8, 128), F32),
        vmem((128, 128), F32),
        vmem((kv_other, 8, 128), F32),
        vmem((128, 128), F32),
        vmem((128, 128), F32),
        vmem((128, 128), F32),
        vmem((128, 128), F32),
        vmem((128, 128), F32),
        vmem((128, 128), F32),
        vmem((16, 384), BF16),
        vmem((kv_other, 16, 384), BF16),
        vmem((8, 128), F32),
        vmem((kv_other, 8, 128), F32),
        vmem((16, 256), BF16),
        vmem((tp_other, 16, 256), BF16),
        vmem((16 * 24, 128), F32),
        vmem((16, 24, 128), BF16),
        vmem((kv_other, 24, 128), BF16),
        vmem((16, 16, 128), BF16),
        vmem((256, 128), F32),
        vmem((2, 16, 128), BF16),
        vmem((tp_other, 16, 128), BF16),
    ]
    scratch += [dma] * 20
    return pl.pallas_call(
        functools.partial(kernel, n_kv, n_tp),
        out_shape=vmem((16, 32), F32),
        in_specs=[pl.BlockSpec(memory_space=pl.ANY)] * len(args),
        scratch_shapes=scratch,
        compiler_params=pltpu.CompilerParams(
            collective_id=0, has_side_effects=True, vmem_limit_bytes=60 * 1024 * 1024
        ),
        name="layer_step",
    )(*args)


def solution(mesh):
    return jax.shard_map(
        functools.partial(on_device, mesh.shape["kv"], mesh.shape["tp"]),
        mesh=mesh,
        in_specs=(
            P(None, ("kv", "tp")),
            P("kv"),
            P("kv", "tp"),
            P("kv", "tp"),
            P("kv", "tp"),
            P("kv", None),
            P("tp"),
            P(None, "kv", "tp"),
            P(None, "kv", "tp"),
            P(None, "tp", "kv"),
            P("tp", "kv"),
            P("kv"),
            P("kv", "tp"),
            P("kv", "tp"),
            P("tp", "kv"),
        ),
        out_specs=P(None, ("kv", "tp")),
        check_vma=False,
    )
```

```python
import functools

import jax
import jax.numpy as jnp
from jax import lax
from jax.experimental import pallas as pl
from jax.experimental.pallas import tpu as pltpu
from jax.sharding import PartitionSpec as P

D = 4096
QH = 48
KEY_VALUE_HEADS = 16
HD = 64
NORM_EPS = 1e-06
MESH = pl.DeviceIdType.MESH
F32 = jnp.float32
BF16 = jnp.bfloat16


def kernel(
    n_kv,
    n_tp,
    hidden_in,
    pre_gain,
    w_query,
    w_key,
    w_value,
    w_forget,
    forget_bias,
    key_cache,
    value_cache,
    decay,
    w_output,
    mid_gain,
    w_gate,
    w_up,
    w_down,
    out_ref,
    xs,
    pg,
    wq,
    wk,
    wv,
    wf,
    fb,
    kc,
    vc,
    dec,
    wo,
    mg,
    wg,
    wu,
    wd,
    load_sem,
    plane,
    dec_rows,
    q_mine,
    q_in,
    q_line,
    u_in,
    s_mine,
    s_in,
    s_line,
    w_in,
    t_mine,
    t_in,
    q_rows,
    o_rows,
    l_rows,
    own_rows,
    top_rows,
    sum_rows,
    a_mine,
    a_in,
    e_mine,
    e_in,
    p_mine,
    p_in,
    g_rows,
    g_mine,
    g_in,
    h_all,
    h_rows,
    d_mine,
    d_in,
    x_send,
    x_recv,
    q_send,
    q_recv,
    u_send,
    u_recv,
    w_send,
    w_recv,
    s_send,
    s_recv,
    t_send,
    t_recv,
    a_send,
    a_recv,
    e_send,
    e_recv,
    p_send,
    p_recv,
    g_send,
    g_recv,
    h_send,
    h_recv,
    d_send,
    d_recv,
):
    kv = lax.axis_index("kv")
    tp = lax.axis_index("tp")
    side = 4
    z, x_at, y, core = kv // side, lax.rem(kv, side), tp // 2, lax.rem(tp, 2)

    def far(d):
        return min(d, side - d)

    steps = [(dz, dx) for dz in range(side) for dx in range(side) if dz or dx]
    steps.sort(key=lambda s: -far(s[0]) - far(s[1]))
    kv_peers = [lax.rem(z + dz, side) * side + lax.rem(x_at + dx, side) for dz, dx in steps]
    steps = [(dy, dc) for dy in range(n_tp // 2) for dc in range(2) if dy or dc]
    steps.sort(key=lambda s: -2 * far(s[0]) - s[1])
    tp_peers = [lax.rem(y + dy, n_tp // 2) * 2 + lax.rem(core + dc, 2) for dy, dc in steps]

    z_line = [lax.rem(z + d, side) * side + x_at for d in (2, 1, 3)]
    x_line = [z * side + lax.rem(x_at + d, side) for d in (2, 1, 3)]
    barrier = pltpu.get_barrier_semaphore()
    for peer in tp_peers:
        pl.semaphore_signal(barrier, inc=1, device_id={"kv": kv, "tp": peer}, device_id_type=MESH)
    for peer in z_line + x_line:
        pl.semaphore_signal(barrier, inc=1, device_id={"kv": peer, "tp": tp}, device_id_type=MESH)

    loads = [
        (hidden_in, xs.at[tp]),
        (pre_gain, pg),
        (w_query, wq),
        (w_key, wk),
        (w_value, wv),
        (w_forget, wf),
        (forget_bias, fb),
        (decay, dec),
        (key_cache, kc),
        (value_cache, vc),
        (w_output, wo),
        (mid_gain, mg),
        (w_gate, wg),
        (w_up, wu),
        (w_down, wd),
    ]
    loads = [pltpu.make_async_copy(a, b, load_sem.at[i]) for i, (a, b) in enumerate(loads)]
    for copy in loads:
        copy.start()
    (l_x, l_pg, l_wq, l_wk, l_wv, l_wf, l_fb, l_dec, l_kc, l_vc, l_wo, l_mg, l_wg, l_wu, l_wd) = loads

    def send(axis, src, dst, landed, send_sem, recv_sem):
        peers = {"kv": kv_peers, "tp": tp_peers, "z": z_line, "x": x_line}[axis]
        for i, peer in enumerate(peers):
            device = {"kv": kv, "tp": peer} if axis == "tp" else {"kv": peer, "tp": tp}
            pltpu.make_async_remote_copy(
                src_ref=src(peer),
                dst_ref=dst(i),
                send_sem=send_sem,
                recv_sem=recv_sem,
                device_id=device,
                device_id_type=MESH,
            ).start()
        return pltpu.make_async_remote_copy(
            src_ref=landed,
            dst_ref=landed,
            send_sem=send_sem,
            recv_sem=recv_sem,
            device_id=device,
            device_id_type=MESH,
        )

    def received(copy):
        copy.wait_recv()

    def sent(copy):
        copy.wait_send()

    lane = lax.broadcasted_iota(jnp.int32, (16, 128), 1)
    low = lane < 64

    pl.semaphore_wait(barrier, n_tp - 1 + len(z_line) + len(x_line))
    for peer in x_line:
        pl.semaphore_signal(plane, inc=1, device_id={"kv": peer, "tp": tp}, device_id_type=MESH)
    l_x.wait()
    x_copies = send("tp", lambda peer: xs.at[tp], lambda i: xs.at[tp], xs.at[pl.ds(0, n_tp - 1)], x_send, x_recv)

    q_rows[...] = jnp.zeros_like(q_rows)
    l_dec.wait()
    row = lax.broadcasted_iota(jnp.int32, (8, 1024), 0)
    for b in range(16):
        dec_rows[b] = jnp.where(row < 3, dec[b, 0:1, :], dec[b, 1:2, :])
    for copy in (l_pg, l_wq, l_wk, l_wv, l_wf, l_fb):
        copy.wait()

    received(x_copies)
    x = jnp.concatenate([xs[t].astype(F32) for t in range(n_tp)], axis=1)
    scaled = (x * pg[...]).astype(BF16)
    q_part = jnp.dot(scaled, wq[...], preferred_element_type=F32)
    q_mine[...] = q_part
    square = jnp.sum(x * x, axis=1, keepdims=True)
    square = jnp.broadcast_to(square, (16, 128))
    s_mine[...] = jnp.where(low[0:8], square[0:8], square[8:16])
    q_copies = send("z", lambda peer: q_mine, lambda i: q_in.at[i], q_in, q_send, q_recv)
    s_copies = send("z", lambda peer: s_mine, lambda i: s_in.at[i], s_in, s_send, s_recv)

    k_part = jnp.dot(scaled, wk[...], preferred_element_type=F32)
    v_part = jnp.dot(scaled, wv[...], preferred_element_type=F32)
    f_part = lax.dot_general(scaled, wf[...], (((1,), (1,)), ((), ())), preferred_element_type=F32)
    f_col = lax.broadcasted_iota(jnp.int32, (16, 16), 1)
    f_zero = jnp.zeros_like(f_part)
    f_first = jnp.sum(jnp.where(f_col == 2 * tp, f_part, f_zero), axis=1, keepdims=True)
    f_second = jnp.sum(jnp.where(f_col == 2 * tp + 1, f_part, f_zero), axis=1, keepdims=True)
    f_wide = jnp.where(low, f_first, f_second)
    t_mine[pl.ds(0, 16, stride=8), :] = k_part
    t_mine[pl.ds(1, 16, stride=8), :] = v_part
    t_mine[pl.ds(2, 16, stride=8), :] = f_wide
    t_mine[pl.ds(3, 16, stride=8), :] = square
    sent(x_copies)
    received(q_copies)
    received(s_copies)
    q_sum = q_mine[...]
    s_sum = s_mine[...]
    for i in range(side - 1):
        q_sum = q_sum + q_in[i]
        s_sum = s_sum + s_in[i]
    q_line[...] = q_sum
    s_line[...] = s_sum
    u_copies = send("x", lambda peer: q_line, lambda i: u_in.at[i], u_in, u_send, u_recv)
    w_copies = send("x", lambda peer: s_line, lambda i: w_in.at[i], w_in, w_send, w_recv)
    pl.semaphore_wait(plane, len(x_line))
    t_copies = send(
        "kv", lambda peer: t_mine.at[pl.ds(pl.multiple_of(peer * 8, 8), 8)], lambda i: t_in.at[i], t_in, t_send, t_recv
    )
    l_kc.wait()
    l_vc.wait()
    sent(q_copies)
    sent(s_copies)

    received(u_copies)
    received(w_copies)
    for i in range(side - 1):
        q_sum = q_sum + u_in[i]
        s_sum = s_sum + w_in[i]
    s_sum = jnp.concatenate([s_sum[:, 0:1], s_sum[:, 64:65]], axis=0)
    inv_rms = lax.rsqrt(s_sum / D + NORM_EPS)
    query = (q_sum * inv_rms).astype(BF16).astype(F32) * (HD**-0.5)
    zero = jnp.zeros((16, 128), F32)
    for h in range(6):
        c, half, g = h // 2, h % 2, h // 3
        part = query[:, c * 128 : (c + 1) * 128]
        if half != g:
            part = pltpu.roll(part, 64, 1)
        q_rows[pl.ds(h, 16, stride=8), :] = jnp.where(low if g == 0 else ~low, part, zero)

    for b in range(16):
        q8 = q_rows[8 * b : 8 * (b + 1), :].astype(BF16)
        scores = lax.dot_general(q8, kc[b], (((1,), (1,)), ((), ())), preferred_element_type=F32)
        scores = scores + dec_rows[b]
        top_rows[8 * b : 8 * (b + 1), :] = functools.reduce(
            jnp.maximum, [scores[:, 128 * j : 128 * (j + 1)] for j in range(8)]
        )
        dec_rows[b] = scores

    received(t_copies)
    t_sum = t_mine[pl.ds(pl.multiple_of(kv * 8, 8), 8), :]
    for i in range(n_kv - 1):
        t_sum = t_sum + t_in[i]
    t_inv = lax.rsqrt(t_sum[3:4, :] / D + NORM_EPS)
    key_new = (t_sum[0:1, :] * t_inv).astype(BF16).astype(F32)
    value_new = (t_sum[1:2, :] * t_inv).astype(BF16).astype(F32)
    low8 = low[0:8]
    row8 = lax.broadcasted_iota(jnp.int32, (8, 128), 0)
    gate_in = t_sum[2:3, :] * t_inv + jnp.where(low[0:1], fb[0:1, 0:1], fb[0:1, 1:2])
    log_new = jnp.minimum(gate_in, 0.0) - jnp.log1p(jnp.exp(-jnp.abs(gate_in)))
    q_own = q_rows[pl.ds(pl.multiple_of(kv * 8, 8), 8), :]
    own = jnp.sum(q_own * key_new, axis=1, keepdims=True)
    own = own - jnp.where(row8[:, 0:1] < 3, log_new[:, 0:1], log_new[:, 64:65])

    own_here = jnp.broadcast_to(own, (8, 128))
    absent = jnp.full((8, 128), -jnp.inf, F32)
    for b in range(16):
        own_rows[8 * b : 8 * (b + 1), :] = jnp.where(kv == b, own_here, absent)
    own_all = own_rows[...]
    top = jnp.maximum(jnp.max(top_rows[...], axis=1, keepdims=True), own_all)
    top_rows[...] = top
    for b in range(16):
        top_b = top_rows[8 * b : 8 * (b + 1), :]
        weights = jnp.exp(dec_rows[b] - jnp.concatenate([top_b] * 8, axis=1))
        sum_rows[8 * b : 8 * (b + 1), :] = functools.reduce(
            jnp.add, [weights[:, 128 * j : 128 * (j + 1)] for j in range(8)]
        )
        o_rows[8 * b : 8 * (b + 1), :] = jnp.dot(weights.astype(BF16), vc[b], preferred_element_type=F32)
    own_weight = jnp.exp(own_all - top)
    total = jnp.sum(sum_rows[...], axis=1, keepdims=True) + own_weight
    o_rows[...] = (o_rows[...] + own_weight * value_new) / total
    l_rows[...] = top + jnp.log(total)

    heads = [o_rows[pl.ds(h, 16, stride=8), :] for h in range(6)]
    logs = [l_rows[pl.ds(h, 16, stride=8), :] for h in range(6)]
    chunk_0 = jnp.where(low, heads[0], pltpu.roll(heads[1], 64, 1))
    chunk_1 = jnp.where(low, heads[2], heads[3])
    chunk_2 = jnp.where(low, pltpu.roll(heads[4], 64, 1), heads[5])
    mine = jnp.concatenate([chunk_0, chunk_1, chunk_2], axis=1).astype(BF16)
    a_mine[...] = mine
    spot = lax.rem(lane, 64)
    e_wide = logs[0]
    for h in range(1, 6):
        e_wide = jnp.where(spot < 8 * h, e_wide, logs[h])
    e_wide = jnp.where(low[0:8], e_wide[0:8], e_wide[8:16])
    e_mine[...] = e_wide
    e_copies = send("kv", lambda peer: e_mine, lambda i: e_in.at[i], e_in, e_send, e_recv)
    a_copies = send("kv", lambda peer: a_mine, lambda i: a_in.at[i], a_in, a_send, a_recv)
    sent(u_copies)
    sent(w_copies)
    sent(t_copies)
    received(e_copies)
    parts = [e_wide] + [e_in[i] for i in range(n_kv - 1)]
    top = functools.reduce(jnp.maximum, parts)
    shares = [jnp.exp(part - top) for part in parts]
    whole = functools.reduce(jnp.add, shares)
    inverse = 1.0 / whole
    l_wo.wait()
    received(a_copies)
    attended = jnp.zeros((16, 384), F32)
    for i in range(n_kv):
        share = shares[i] * inverse
        wide = [
            jnp.concatenate([jnp.broadcast_to(share[:, at : at + 1], (8, 128)) for at in (8 * h, 64 + 8 * h)], axis=0)
            for h in range(6)
        ]
        wide = jnp.concatenate([jnp.where(low, wide[2 * c], wide[2 * c + 1]) for c in range(3)], axis=1)
        value = mine if i == 0 else a_in[i - 1]
        attended = attended + wide * value.astype(F32)

    part = jnp.dot(attended.astype(BF16), wo[...], preferred_element_type=F32).astype(BF16)
    p_mine[...] = part
    p_copies = send("tp", lambda peer: p_mine, lambda i: p_in.at[i], p_in, p_send, p_recv)
    sent(e_copies)
    sent(a_copies)
    for copy in (l_mg, l_wg, l_wu, l_wd):
        copy.wait()
    received(p_copies)
    projected = part.astype(F32)
    for i in range(n_tp - 1):
        projected = projected + p_in[i].astype(F32)
    mid = x + projected
    mid_scaled = (mid * mg[...]).astype(BF16)
    gate_part = jnp.dot(mid_scaled, wg[...], preferred_element_type=F32)
    up_part = jnp.dot(mid_scaled, wu[...], preferred_element_type=F32)
    mid_square = jnp.broadcast_to(jnp.sum(mid * mid, axis=1, keepdims=True), (16, 128))
    square_high = mid_square.astype(BF16).astype(F32)
    for c in range(11):
        g_rows[pl.ds(c, 16, stride=24), :] = gate_part[:, 128 * c : 128 * (c + 1)]
        g_rows[pl.ds(11 + c, 16, stride=24), :] = up_part[:, 128 * c : 128 * (c + 1)]
    g_rows[pl.ds(22, 16, stride=24), :] = square_high
    g_rows[pl.ds(23, 16, stride=24), :] = mid_square - square_high
    for b in range(16):
        g_mine[b] = g_rows[24 * b : 24 * (b + 1), :].astype(BF16)
    g_copies = send("kv", lambda peer: g_mine.at[peer], lambda i: g_in.at[i], g_in, g_send, g_recv)
    sent(p_copies)
    received(g_copies)
    g_sum = g_mine[kv].astype(F32)
    for i in range(n_kv - 1):
        g_sum = g_sum + g_in[i].astype(F32)
    mid_inv = lax.rsqrt((g_sum[22:23, :] + g_sum[23:24, :]) / D + NORM_EPS)
    gate = g_sum[0:11, :] * mid_inv
    up = g_sum[11:22, :] * mid_inv
    hidden = gate / (1.0 + jnp.exp(-gate)) * up
    hidden = jnp.concatenate([hidden, jnp.zeros((5, 128), F32)], axis=0).astype(BF16)
    h_all[kv] = hidden
    h_copies = send("kv", lambda peer: h_all.at[kv], lambda i: h_all.at[kv], h_all.at[pl.ds(0, n_kv - 1)], h_send, h_recv)
    sent(g_copies)
    received(h_copies)
    for b in range(16):
        h_rows[16 * b : 16 * (b + 1), :] = h_all[b].astype(F32)
    units = jnp.concatenate([h_rows[pl.ds(c, 16, stride=16), :] for c in range(11)], axis=1).astype(BF16)
    down = jnp.dot(units, wd[...], preferred_element_type=F32).astype(BF16)
    d_mine[0] = down[:, 0:128]
    d_mine[1] = down[:, 128:256]
    d_copies = send("tp", lambda peer: d_mine.at[peer // 4], lambda i: d_in.at[i], d_in, d_send, d_recv)
    sent(h_copies)
    result = d_mine[tp // 4].astype(F32)
    received(d_copies)
    for i in range(n_tp - 1):
        result = result + d_in[i].astype(F32)
    result = jnp.where(tp < 4, mid[:, 0:128], mid[:, 128:256]) + result
    place = lax.rem(tp, 4)
    pick = result[:, 0:32]
    for r in range(1, 4):
        pick = jnp.where(place == r, result[:, 32 * r : 32 * (r + 1)], pick)
    out_ref[...] = pick
    sent(d_copies)


def on_device(n_kv, n_tp, *args):
    args = list(args)
    for i in (1, 6, 11):
        args[i] = args[i].reshape(1, -1)
    args[5] = args[5].T
    vmem = pltpu.VMEM
    own = [vmem(a.shape, a.dtype) for a in args[1:]]
    kv_other, tp_other = n_kv - 1, n_tp - 1
    dma = pltpu.SemaphoreType.DMA
    scratch = [
        vmem((n_tp, 16, 32), BF16),
        *own,
        dma((15,)),
        pltpu.SemaphoreType.REGULAR,
        vmem((16, 8, 1024), F32),
        vmem((16, 384), F32),
        vmem((3, 16, 384), F32),
        vmem((16, 384), F32),
        vmem((3, 16, 384), F32),
        vmem((8, 128), F32),
        vmem((3, 8, 128), F32),
        vmem((8, 128), F32),
        vmem((3, 8, 128), F32),
        vmem((128, 128), F32),
        vmem((kv_other, 8, 128), F32),
        vmem((128, 128), F32),
        vmem((128, 128), F32),
        vmem((128, 128), F32),
        vmem((128, 128), F32),
        vmem((128, 128), F32),
        vmem((128, 128), F32),
        vmem((16, 384), BF16),
        vmem((kv_other, 16, 384), BF16),
        vmem((8, 128), F32),
        vmem((kv_other, 8, 128), F32),
        vmem((16, 256), BF16),
        vmem((tp_other, 16, 256), BF16),
        vmem((16 * 24, 128), F32),
        vmem((16, 24, 128), BF16),
        vmem((kv_other, 24, 128), BF16),
        vmem((16, 16, 128), BF16),
        vmem((256, 128), F32),
        vmem((2, 16, 128), BF16),
        vmem((tp_other, 16, 128), BF16),
    ]
    scratch += [dma] * 24
    return pl.pallas_call(
        functools.partial(kernel, n_kv, n_tp),
        out_shape=vmem((16, 32), F32),
        in_specs=[pl.BlockSpec(memory_space=pl.ANY)] * len(args),
        scratch_shapes=scratch,
        compiler_params=pltpu.CompilerParams(
            collective_id=0, has_side_effects=True, vmem_limit_bytes=60 * 1024 * 1024
        ),
        name="layer_step",
    )(*args)


def solution(mesh):
    return jax.shard_map(
        functools.partial(on_device, mesh.shape["kv"], mesh.shape["tp"]),
        mesh=mesh,
        in_specs=(
            P(None, ("kv", "tp")),
            P("kv"),
            P("kv", "tp"),
            P("kv", "tp"),
            P("kv", "tp"),
            P("kv", None),
            P("tp"),
            P(None, "kv", "tp"),
            P(None, "kv", "tp"),
            P(None, "tp", "kv"),
            P("tp", "kv"),
            P("kv"),
            P("kv", "tp"),
            P("kv", "tp"),
            P("tp", "kv"),
        ),
        out_specs=P(None, ("kv", "tp")),
        check_vma=False,
    )
```

```python
import functools

import jax
import jax.numpy as jnp
from jax import lax
from jax.experimental import pallas as pl
from jax.experimental.pallas import tpu as pltpu
from jax.sharding import PartitionSpec as P

D = 4096
QH = 48
KEY_VALUE_HEADS = 16
HD = 64
NORM_EPS = 1e-06
MESH = pl.DeviceIdType.MESH
F32 = jnp.float32
BF16 = jnp.bfloat16


def kernel(
    n_kv,
    n_tp,
    hidden_in,
    pre_gain,
    w_query,
    w_key,
    w_value,
    w_forget,
    forget_bias,
    key_cache,
    value_cache,
    decay,
    w_output,
    mid_gain,
    w_gate,
    w_up,
    w_down,
    out_ref,
    xs,
    pg,
    wq,
    wk,
    wv,
    wf,
    fb,
    kc,
    vc,
    dec,
    wo,
    mg,
    wg,
    wu,
    wd,
    load_sem,
    plane,
    dec_rows,
    q_mine,
    q_in,
    q_line,
    u_in,
    s_mine,
    s_in,
    s_line,
    w_in,
    t_mine,
    t_in,
    q_rows,
    o_rows,
    l_rows,
    own_rows,
    top_rows,
    sum_rows,
    w_rows,
    a_mine,
    a_in,
    e_mine,
    e_in,
    p_mine,
    p_in,
    g_rows,
    g_mine,
    g_in,
    h_all,
    h_rows,
    d_mine,
    d_in,
    x_send,
    x_recv,
    q_send,
    q_recv,
    u_send,
    u_recv,
    w_send,
    w_recv,
    s_send,
    s_recv,
    t_send,
    t_recv,
    a_send,
    a_recv,
    e_send,
    e_recv,
    p_send,
    p_recv,
    g_send,
    g_recv,
    h_send,
    h_recv,
    d_send,
    d_recv,
):
    kv = lax.axis_index("kv")
    tp = lax.axis_index("tp")
    side = 4
    z, x_at, y, core = kv // side, lax.rem(kv, side), tp // 2, lax.rem(tp, 2)

    def far(d):
        return min(d, side - d)

    steps = [(dz, dx) for dz in range(side) for dx in range(side) if dz or dx]
    steps.sort(key=lambda s: -far(s[0]) - far(s[1]))
    kv_peers = [lax.rem(z + dz, side) * side + lax.rem(x_at + dx, side) for dz, dx in steps]
    steps = [(dy, dc) for dy in range(n_tp // 2) for dc in range(2) if dy or dc]
    steps.sort(key=lambda s: -2 * far(s[0]) - s[1])
    tp_peers = [lax.rem(y + dy, n_tp // 2) * 2 + lax.rem(core + dc, 2) for dy, dc in steps]

    z_line = [lax.rem(z + d, side) * side + x_at for d in (2, 1, 3)]
    x_line = [z * side + lax.rem(x_at + d, side) for d in (2, 1, 3)]
    barrier = pltpu.get_barrier_semaphore()
    for peer in tp_peers:
        pl.semaphore_signal(barrier, inc=1, device_id={"kv": kv, "tp": peer}, device_id_type=MESH)
    for peer in z_line + x_line:
        pl.semaphore_signal(barrier, inc=1, device_id={"kv": peer, "tp": tp}, device_id_type=MESH)

    loads = [
        (hidden_in, xs.at[tp]),
        (pre_gain, pg),
        (w_query, wq),
        (w_key, wk),
        (w_value, wv),
        (w_forget, wf),
        (forget_bias, fb),
        (decay, dec),
        (key_cache, kc),
        (value_cache, vc),
        (w_output, wo),
        (mid_gain, mg),
        (w_gate, wg),
        (w_up, wu),
        (w_down, wd),
    ]
    loads = [pltpu.make_async_copy(a, b, load_sem.at[i]) for i, (a, b) in enumerate(loads)]
    for copy in loads:
        copy.start()
    (l_x, l_pg, l_wq, l_wk, l_wv, l_wf, l_fb, l_dec, l_kc, l_vc, l_wo, l_mg, l_wg, l_wu, l_wd) = loads

    def send(axis, src, dst, landed, send_sem, recv_sem):
        peers = {"kv": kv_peers, "tp": tp_peers, "z": z_line, "x": x_line}[axis]
        for i, peer in enumerate(peers):
            device = {"kv": kv, "tp": peer} if axis == "tp" else {"kv": peer, "tp": tp}
            pltpu.make_async_remote_copy(
                src_ref=src(peer),
                dst_ref=dst(i),
                send_sem=send_sem,
                recv_sem=recv_sem,
                device_id=device,
                device_id_type=MESH,
            ).start()
        return pltpu.make_async_remote_copy(
            src_ref=landed,
            dst_ref=landed,
            send_sem=send_sem,
            recv_sem=recv_sem,
            device_id=device,
            device_id_type=MESH,
        )

    def received(copy):
        copy.wait_recv()

    def sent(copy):
        copy.wait_send()

    lane = lax.broadcasted_iota(jnp.int32, (16, 128), 1)
    low = lane < 64

    pl.semaphore_wait(barrier, n_tp - 1 + len(z_line) + len(x_line))
    for peer in x_line:
        pl.semaphore_signal(plane, inc=1, device_id={"kv": peer, "tp": tp}, device_id_type=MESH)
    l_x.wait()
    x_copies = send("tp", lambda peer: xs.at[tp], lambda i: xs.at[tp], xs.at[pl.ds(0, n_tp - 1)], x_send, x_recv)

    q_rows[...] = jnp.zeros_like(q_rows)
    l_dec.wait()
    row = lax.broadcasted_iota(jnp.int32, (8, 1024), 0)
    for b in range(16):
        dec_rows[b] = jnp.where(row < 3, dec[b, 0:1, :], dec[b, 1:2, :])
    for copy in (l_pg, l_wq, l_wk, l_wv, l_wf, l_fb):
        copy.wait()

    received(x_copies)
    x = jnp.concatenate([xs[t].astype(F32) for t in range(n_tp)], axis=1)
    scaled = (x * pg[...]).astype(BF16)
    q_part = jnp.dot(scaled, wq[...], preferred_element_type=F32)
    q_mine[...] = q_part
    square = jnp.sum(x * x, axis=1, keepdims=True)
    square = jnp.broadcast_to(square, (16, 128))
    s_mine[...] = jnp.where(low[0:8], square[0:8], square[8:16])
    q_copies = send("z", lambda peer: q_mine, lambda i: q_in.at[i], q_in, q_send, q_recv)
    s_copies = send("z", lambda peer: s_mine, lambda i: s_in.at[i], s_in, s_send, s_recv)

    k_part = jnp.dot(scaled, wk[...], preferred_element_type=F32)
    v_part = jnp.dot(scaled, wv[...], preferred_element_type=F32)
    f_part = lax.dot_general(scaled, wf[...], (((1,), (1,)), ((), ())), preferred_element_type=F32)
    f_col = lax.broadcasted_iota(jnp.int32, (16, 16), 1)
    f_zero = jnp.zeros_like(f_part)
    f_first = jnp.sum(jnp.where(f_col == 2 * tp, f_part, f_zero), axis=1, keepdims=True)
    f_second = jnp.sum(jnp.where(f_col == 2 * tp + 1, f_part, f_zero), axis=1, keepdims=True)
    f_wide = jnp.where(low, f_first, f_second)
    t_mine[pl.ds(0, 16, stride=8), :] = k_part
    t_mine[pl.ds(1, 16, stride=8), :] = v_part
    t_mine[pl.ds(2, 16, stride=8), :] = f_wide
    t_mine[pl.ds(3, 16, stride=8), :] = square
    sent(x_copies)
    received(q_copies)
    received(s_copies)
    q_sum = q_mine[...]
    s_sum = s_mine[...]
    for i in range(side - 1):
        q_sum = q_sum + q_in[i]
        s_sum = s_sum + s_in[i]
    q_line[...] = q_sum
    s_line[...] = s_sum
    u_copies = send("x", lambda peer: q_line, lambda i: u_in.at[i], u_in, u_send, u_recv)
    w_copies = send("x", lambda peer: s_line, lambda i: w_in.at[i], w_in, w_send, w_recv)
    pl.semaphore_wait(plane, len(x_line))
    t_copies = send(
        "kv", lambda peer: t_mine.at[pl.ds(pl.multiple_of(peer * 8, 8), 8)], lambda i: t_in.at[i], t_in, t_send, t_recv
    )
    l_kc.wait()
    l_vc.wait()
    sent(q_copies)
    sent(s_copies)

    received(u_copies)
    received(w_copies)
    for i in range(side - 1):
        q_sum = q_sum + u_in[i]
        s_sum = s_sum + w_in[i]
    s_sum = jnp.concatenate([s_sum[:, 0:1], s_sum[:, 64:65]], axis=0)
    inv_rms = lax.rsqrt(s_sum / D + NORM_EPS)
    query = (q_sum * inv_rms).astype(BF16).astype(F32) * (HD**-0.5)
    zero = jnp.zeros((16, 128), F32)
    for h in range(6):
        c, half, g = h // 2, h % 2, h // 3
        part = query[:, c * 128 : (c + 1) * 128]
        if half != g:
            part = pltpu.roll(part, 64, 1)
        q_rows[pl.ds(h, 16, stride=8), :] = jnp.where(low if g == 0 else ~low, part, zero)

    for b in range(16):
        q8 = q_rows[8 * b : 8 * (b + 1), :].astype(BF16)
        scores = lax.dot_general(q8, kc[b], (((1,), (1,)), ((), ())), preferred_element_type=F32)
        scores = scores + dec_rows[b]
        top_rows[8 * b : 8 * (b + 1), :] = functools.reduce(
            jnp.maximum, [scores[:, 128 * j : 128 * (j + 1)] for j in range(8)]
        )
        dec_rows[b] = scores

    received(t_copies)
    t_sum = t_mine[pl.ds(pl.multiple_of(kv * 8, 8), 8), :]
    for i in range(n_kv - 1):
        t_sum = t_sum + t_in[i]
    t_inv = lax.rsqrt(t_sum[3:4, :] / D + NORM_EPS)
    key_new = (t_sum[0:1, :] * t_inv).astype(BF16).astype(F32)
    value_new = (t_sum[1:2, :] * t_inv).astype(BF16).astype(F32)
    low8 = low[0:8]
    row8 = lax.broadcasted_iota(jnp.int32, (8, 128), 0)
    gate_in = t_sum[2:3, :] * t_inv + jnp.where(low[0:1], fb[0:1, 0:1], fb[0:1, 1:2])
    log_new = jnp.minimum(gate_in, 0.0) - jnp.log1p(jnp.exp(-jnp.abs(gate_in)))
    q_own = q_rows[pl.ds(pl.multiple_of(kv * 8, 8), 8), :]
    own = jnp.sum(q_own * key_new, axis=1, keepdims=True)
    own = own - jnp.where(row8[:, 0:1] < 3, log_new[:, 0:1], log_new[:, 64:65])

    own_here = jnp.broadcast_to(own, (8, 128))
    absent = jnp.full((8, 128), -jnp.inf, F32)
    for b in range(16):
        own_rows[8 * b : 8 * (b + 1), :] = jnp.where(kv == b, own_here, absent)
    own_all = own_rows[...]
    top = jnp.maximum(jnp.max(top_rows[...], axis=1, keepdims=True), own_all)
    top_rows[...] = top
    for b in range(16):
        top_b = top_rows[8 * b : 8 * (b + 1), :]
        weights = jnp.exp(dec_rows[b] - jnp.concatenate([top_b] * 8, axis=1))
        sum_rows[8 * b : 8 * (b + 1), :] = functools.reduce(
            jnp.add, [weights[:, 128 * j : 128 * (j + 1)] for j in range(8)]
        )
        w_rows[b] = weights.astype(BF16)
    own_weight = jnp.exp(own_all - top)
    total = jnp.sum(sum_rows[...], axis=1, keepdims=True) + own_weight
    l_rows[...] = top + jnp.log(total)
    logs = [l_rows[pl.ds(h, 16, stride=8), :] for h in range(6)]
    spot = lax.rem(lane, 64)
    e_wide = logs[0]
    for h in range(1, 6):
        e_wide = jnp.where(spot < 8 * h, e_wide, logs[h])
    e_wide = jnp.where(low[0:8], e_wide[0:8], e_wide[8:16])
    e_mine[...] = e_wide
    e_copies = send("kv", lambda peer: e_mine, lambda i: e_in.at[i], e_in, e_send, e_recv)
    for b in range(16):
        o_rows[8 * b : 8 * (b + 1), :] = jnp.dot(w_rows[b], vc[b], preferred_element_type=F32)
    o_rows[...] = (o_rows[...] + own_weight * value_new) / total

    heads = [o_rows[pl.ds(h, 16, stride=8), :] for h in range(6)]
    chunk_0 = jnp.where(low, heads[0], pltpu.roll(heads[1], 64, 1))
    chunk_1 = jnp.where(low, heads[2], heads[3])
    chunk_2 = jnp.where(low, pltpu.roll(heads[4], 64, 1), heads[5])
    mine = jnp.concatenate([chunk_0, chunk_1, chunk_2], axis=1).astype(BF16)
    a_mine[...] = mine
    a_copies = send("kv", lambda peer: a_mine, lambda i: a_in.at[i], a_in, a_send, a_recv)
    sent(u_copies)
    sent(w_copies)
    sent(t_copies)
    received(e_copies)
    parts = [e_wide] + [e_in[i] for i in range(n_kv - 1)]
    top = functools.reduce(jnp.maximum, parts)
    shares = [jnp.exp(part - top) for part in parts]
    whole = functools.reduce(jnp.add, shares)
    inverse = 1.0 / whole
    l_wo.wait()
    received(a_copies)
    attended = jnp.zeros((16, 384), F32)
    for i in range(n_kv):
        share = shares[i] * inverse
        wide = [
            jnp.concatenate([jnp.broadcast_to(share[:, at : at + 1], (8, 128)) for at in (8 * h, 64 + 8 * h)], axis=0)
            for h in range(6)
        ]
        wide = jnp.concatenate([jnp.where(low, wide[2 * c], wide[2 * c + 1]) for c in range(3)], axis=1)
        value = mine if i == 0 else a_in[i - 1]
        attended = attended + wide * value.astype(F32)

    part = jnp.dot(attended.astype(BF16), wo[...], preferred_element_type=F32).astype(BF16)
    p_mine[...] = part
    p_copies = send("tp", lambda peer: p_mine, lambda i: p_in.at[i], p_in, p_send, p_recv)
    sent(e_copies)
    sent(a_copies)
    for copy in (l_mg, l_wg, l_wu, l_wd):
        copy.wait()
    received(p_copies)
    projected = part.astype(F32)
    for i in range(n_tp - 1):
        projected = projected + p_in[i].astype(F32)
    mid = x + projected
    mid_scaled = (mid * mg[...]).astype(BF16)
    gate_part = jnp.dot(mid_scaled, wg[...], preferred_element_type=F32)
    up_part = jnp.dot(mid_scaled, wu[...], preferred_element_type=F32)
    mid_square = jnp.broadcast_to(jnp.sum(mid * mid, axis=1, keepdims=True), (16, 128))
    square_high = mid_square.astype(BF16).astype(F32)
    for c in range(11):
        g_rows[pl.ds(c, 16, stride=24), :] = gate_part[:, 128 * c : 128 * (c + 1)]
        g_rows[pl.ds(11 + c, 16, stride=24), :] = up_part[:, 128 * c : 128 * (c + 1)]
    g_rows[pl.ds(22, 16, stride=24), :] = square_high
    g_rows[pl.ds(23, 16, stride=24), :] = mid_square - square_high
    for b in range(16):
        g_mine[b] = g_rows[24 * b : 24 * (b + 1), :].astype(BF16)
    g_copies = send("kv", lambda peer: g_mine.at[peer], lambda i: g_in.at[i], g_in, g_send, g_recv)
    sent(p_copies)
    received(g_copies)
    g_sum = g_mine[kv].astype(F32)
    for i in range(n_kv - 1):
        g_sum = g_sum + g_in[i].astype(F32)
    mid_inv = lax.rsqrt((g_sum[22:23, :] + g_sum[23:24, :]) / D + NORM_EPS)
    gate = g_sum[0:11, :] * mid_inv
    up = g_sum[11:22, :] * mid_inv
    hidden = gate / (1.0 + jnp.exp(-gate)) * up
    hidden = jnp.concatenate([hidden, jnp.zeros((5, 128), F32)], axis=0).astype(BF16)
    h_all[kv] = hidden
    h_copies = send("kv", lambda peer: h_all.at[kv], lambda i: h_all.at[kv], h_all.at[pl.ds(0, n_kv - 1)], h_send, h_recv)
    sent(g_copies)
    received(h_copies)
    for b in range(16):
        h_rows[16 * b : 16 * (b + 1), :] = h_all[b].astype(F32)
    units = jnp.concatenate([h_rows[pl.ds(c, 16, stride=16), :] for c in range(11)], axis=1).astype(BF16)
    down = jnp.dot(units, wd[...], preferred_element_type=F32).astype(BF16)
    d_mine[0] = down[:, 0:128]
    d_mine[1] = down[:, 128:256]
    d_copies = send("tp", lambda peer: d_mine.at[peer // 4], lambda i: d_in.at[i], d_in, d_send, d_recv)
    sent(h_copies)
    result = d_mine[tp // 4].astype(F32)
    received(d_copies)
    for i in range(n_tp - 1):
        result = result + d_in[i].astype(F32)
    result = jnp.where(tp < 4, mid[:, 0:128], mid[:, 128:256]) + result
    place = lax.rem(tp, 4)
    pick = result[:, 0:32]
    for r in range(1, 4):
        pick = jnp.where(place == r, result[:, 32 * r : 32 * (r + 1)], pick)
    out_ref[...] = pick
    sent(d_copies)


def on_device(n_kv, n_tp, *args):
    args = list(args)
    for i in (1, 6, 11):
        args[i] = args[i].reshape(1, -1)
    args[5] = args[5].T
    vmem = pltpu.VMEM
    own = [vmem(a.shape, a.dtype) for a in args[1:]]
    kv_other, tp_other = n_kv - 1, n_tp - 1
    dma = pltpu.SemaphoreType.DMA
    scratch = [
        vmem((n_tp, 16, 32), BF16),
        *own,
        dma((15,)),
        pltpu.SemaphoreType.REGULAR,
        vmem((16, 8, 1024), F32),
        vmem((16, 384), F32),
        vmem((3, 16, 384), F32),
        vmem((16, 384), F32),
        vmem((3, 16, 384), F32),
        vmem((8, 128), F32),
        vmem((3, 8, 128), F32),
        vmem((8, 128), F32),
        vmem((3, 8, 128), F32),
        vmem((128, 128), F32),
        vmem((kv_other, 8, 128), F32),
        vmem((128, 128), F32),
        vmem((128, 128), F32),
        vmem((128, 128), F32),
        vmem((128, 128), F32),
        vmem((128, 128), F32),
        vmem((128, 128), F32),
        vmem((16, 8, 1024), BF16),
        vmem((16, 384), BF16),
        vmem((kv_other, 16, 384), BF16),
        vmem((8, 128), F32),
        vmem((kv_other, 8, 128), F32),
        vmem((16, 256), BF16),
        vmem((tp_other, 16, 256), BF16),
        vmem((16 * 24, 128), F32),
        vmem((16, 24, 128), BF16),
        vmem((kv_other, 24, 128), BF16),
        vmem((16, 16, 128), BF16),
        vmem((256, 128), F32),
        vmem((2, 16, 128), BF16),
        vmem((tp_other, 16, 128), BF16),
    ]
    scratch += [dma] * 24
    return pl.pallas_call(
        functools.partial(kernel, n_kv, n_tp),
        out_shape=vmem((16, 32), F32),
        in_specs=[pl.BlockSpec(memory_space=pl.ANY)] * len(args),
        scratch_shapes=scratch,
        compiler_params=pltpu.CompilerParams(
            collective_id=0, has_side_effects=True, vmem_limit_bytes=60 * 1024 * 1024
        ),
        name="layer_step",
    )(*args)


def solution(mesh):
    return jax.shard_map(
        functools.partial(on_device, mesh.shape["kv"], mesh.shape["tp"]),
        mesh=mesh,
        in_specs=(
            P(None, ("kv", "tp")),
            P("kv"),
            P("kv", "tp"),
            P("kv", "tp"),
            P("kv", "tp"),
            P("kv", None),
            P("tp"),
            P(None, "kv", "tp"),
            P(None, "kv", "tp"),
            P(None, "tp", "kv"),
            P("tp", "kv"),
            P("kv"),
            P("kv", "tp"),
            P("kv", "tp"),
            P("tp", "kv"),
        ),
        out_specs=P(None, ("kv", "tp")),
        check_vma=False,
    )
```
